32 devices in a mesh: sp: 4 (over z), fs: 2 (over y), tp: 4 (over x, core).
Axes of the slice: x: 2, y: 2, z: 4, core: 2. Of those that a mesh axis runs over, the one named last changes fastest.
Arguments:
- tokens: bfloat16 [2, 3072, 2304], P('fs', 'sp'), may hold values from -6 to 6
- norm_gain: float32 [2304], replicated, may hold values from 0.1 to 1.9
- query_weight: bfloat16 [2304, 2048], P(('sp', 'fs'), 'tp'), may hold values from -6 to 6
- key_weight: bfloat16 [2304, 512], P(('sp', 'fs'), 'tp'), may hold values from -6 to 6
- value_weight: bfloat16 [2304, 512], P(('sp', 'fs'), 'tp'), may hold values from -0.125 to 0.125
- outer_weight: bfloat16 [2304, 2048], P(('sp', 'fs'), 'tp'), may hold values from -0.125 to 0.125
- inner_weight: bfloat16 [2304, 2048], P(('sp', 'fs'), 'tp'), may hold values from -0.125 to 0.125
- signal_weight: bfloat16 [2304, 2048], P(('sp', 'fs'), 'tp'), may hold values from -0.125 to 0.125
- conv_taps: float32 [3, 2048], P(None, 'tp'), may hold values from -3 to 3
- sink_logit: float32 [32], P('tp'), may hold values from -4 to 4
Outputs:
- attn_out: bfloat16 [2, 3072, 2048], P('fs', 'sp', 'tp')
- conv_out: bfloat16 [2, 3072, 2048], P('fs', 'sp', 'tp')
- log_total: float32 [2, 32, 3072], P('fs', 'tp', 'sp')
The draws below stay inside these ranges and needn't reach their ends.
All inputs are finite; a program needn't handle non-finite values.
Results may differ from the reference program's by a relative error of at most 0.014.
The reference program's roundings to bfloat16 on the way (of `normed`, `product` and `rounded`) count: a program that leaves them out, or rounds other values in their place, can miss the bound.
Values may be sent and summed in bfloat16 or wider, within the bound.
No kernel may reach another device: no remote copies, remote signals or barrier semaphores. Data moves between devices by JAX's collectives and lax.ppermute only.
A program may use at most 64 MiB of HBM per device.

```python
import math
import jax
import jax.numpy as jnp
from jax import lax

D = 2304
HEAD = 64
QHEADS = 32
KVHEADS = 8
CHANNELS = 2048
WINDOW = 128
SEQS = 2
LEN = 3072


def draw_tokens(key, part):
    base = jax.random.normal(jax.random.fold_in(key, 3), (SEQS, LEN, D), jnp.float32)
    return jnp.clip(base, -6.0, 6.0).astype(jnp.bfloat16)


def projection_pair(key):
    scaling = 1.0 / math.sqrt(D)
    query_base = jax.random.normal(jax.random.fold_in(key, 21), (D, QHEADS * HEAD), jnp.float32) * scaling
    key_base = jax.random.normal(jax.random.fold_in(key, 22), (D, KVHEADS * HEAD), jnp.float32) * scaling
    return (jnp.clip(query_base, -6.0, 6.0), jnp.clip(key_base, -6.0, 6.0))


def draw_query_weight(key, part):
    return projection_pair(key)[0].astype(jnp.bfloat16)


def draw_key_weight(key, part):
    return projection_pair(key)[1].astype(jnp.bfloat16)


def block_scale(own_key, shape, shards, smallest, top_value):
    gain, own = 1.0, jax.random.fold_in(own_key, 6)
    for position, blocks in shards:
        draws = jnp.exp(jax.random.uniform(jax.random.fold_in(own, position), (blocks,), jnp.float32, smallest / len(shards), top_value / len(shards)))
        gain = gain * jnp.repeat(draws, shape[position] // blocks).reshape([-1 if axis == position else 1 for axis in range(len(shape))])
    return gain


def normal_values(own_key, dims, scale, reach, cuts=(), held_as=jnp.bfloat16):
    drawn = scale * jax.random.normal(own_key, dims, jnp.float32)
    if cuts:
        drawn = drawn * block_scale(own_key, dims, cuts, -0.22, 0.18)
    return jnp.clip(drawn, -reach, reach).astype(held_as)


def setup_inputs(seed: int = 0) -> dict:
    splits = jax.random.split(jax.random.key(seed), 11)
    return {
        "tokens": draw_tokens(jax.random.fold_in(splits[10], 71), 0),
        "norm_gain": jnp.clip(1.0 + 0.18 * jax.random.normal(splits[1], (D,), jnp.float32), 0.1, 1.9),
        "query_weight": draw_query_weight(jax.random.fold_in(splits[10], 71), 0),
        "key_weight": draw_key_weight(jax.random.fold_in(splits[10], 71), 0),
        "value_weight": normal_values(splits[4], (D, KVHEADS * HEAD), D ** -0.5, 0.125, ((0, 8), (1, 4))),
        "outer_weight": normal_values(splits[5], (D, CHANNELS), D ** -0.5, 0.125, ((0, 8), (1, 4))),
        "inner_weight": normal_values(splits[6], (D, CHANNELS), D ** -0.5, 0.125, ((0, 8), (1, 4))),
        "signal_weight": normal_values(splits[7], (D, CHANNELS), D ** -0.5, 0.125, ((0, 8), (1, 4))),
        "conv_taps": normal_values(splits[8], (3, CHANNELS), 0.6, 3.0, ((1, 4),), jnp.float32),
        "sink_logit": normal_values(splits[9], (QHEADS,), 1.5, 4.0, ((0, 4),), jnp.float32),
    }


EPSILON = 1e-06

def normalized(tokens, norm_gain):
    values = tokens.astype(jnp.float32)
    scaling = lax.rsqrt(lax.optimization_barrier(jnp.mean(values * values, axis=-1, keepdims=True)) + EPSILON)
    return (values * scaling * norm_gain).astype(jnp.bfloat16)

def banded_attention(queries, key_proj, value_proj, sink_logit):
    seq_length = queries.shape[0]
    group_size = QHEADS // KVHEADS
    block_count = seq_length // WINDOW
    query_blocks = queries.astype(jnp.float32).reshape(block_count, WINDOW, KVHEADS, group_size, HEAD)
    key_rows = jnp.pad(key_proj.astype(jnp.float32), ((WINDOW, WINDOW), (0, 0))).reshape(block_count + 2, WINDOW, KVHEADS, HEAD)
    value_rows = jnp.pad(value_proj.astype(jnp.float32), ((WINDOW, WINDOW), (0, 0))).reshape(block_count + 2, WINDOW, KVHEADS, HEAD)
    key_span = jnp.concatenate([key_rows[:-2], key_rows[1:-1], key_rows[2:]], axis=1)
    value_span = jnp.concatenate([value_rows[:-2], value_rows[1:-1], value_rows[2:]], axis=1)
    scores = jnp.einsum('bqkgd,bskd->bkgqs', query_blocks, key_span) * (1.0 / math.sqrt(HEAD))
    distance = jnp.arange(WINDOW)[:, None] - jnp.arange(3 * WINDOW)[None, :] + WINDOW
    key_pos = WINDOW * jnp.arange(block_count)[:, None] - WINDOW + jnp.arange(3 * WINDOW)[None, :]
    inside = (jnp.abs(distance)[None] <= WINDOW) & ((key_pos >= 0) & (key_pos < seq_length))[:, None, :]
    slopes = jnp.exp2(-8.0 * jnp.arange(1, QHEADS + 1, dtype=jnp.float32) / QHEADS)
    scores = scores - slopes.reshape(KVHEADS, group_size, 1, 1) * jnp.abs(distance).astype(jnp.float32)
    scores = jnp.where(inside[:, None, None], scores, -jnp.inf)
    sink_grid = sink_logit.reshape(KVHEADS, group_size, 1, 1)
    row_peak = jnp.maximum(lax.optimization_barrier(jnp.max(scores, axis=-1, keepdims=True)), sink_grid)
    weights = jnp.exp(scores - row_peak)
    row_total = lax.optimization_barrier(jnp.sum(weights, axis=-1, keepdims=True)) + jnp.exp(sink_grid - row_peak)
    rounded = lax.optimization_barrier(weights.astype(jnp.bfloat16)).astype(jnp.float32)
    weighted = jnp.einsum('bkgqs,bskd->bqkgd', rounded, value_span)
    attended = (weighted / row_total.transpose(0, 3, 1, 2, 4)).astype(jnp.bfloat16).reshape(seq_length, QHEADS * HEAD)
    log_total = (row_peak + jnp.log(row_total))[..., 0].transpose(1, 2, 0, 3).reshape(QHEADS, seq_length)
    return (attended, log_total)

def reference(tokens, norm_gain, query_weight, key_weight, value_weight, outer_weight, inner_weight, signal_weight, conv_taps, sink_logit):

    def one_sequence(rows_in):
        normed = normalized(rows_in, norm_gain)

        def project(weight):
            return jnp.dot(normed, weight, preferred_element_type=jnp.float32).astype(jnp.bfloat16)
        queries = project(query_weight)
        key_proj = project(key_weight)
        value_proj = project(value_weight)
        outer_gate = project(outer_weight)
        inner_gate = project(inner_weight)
        signal = project(signal_weight)
        product = (inner_gate.astype(jnp.float32) * signal.astype(jnp.float32)).astype(jnp.bfloat16)
        padded = jnp.pad(product, ((1, 1), (0, 0))).astype(jnp.float32)
        mixed_conv = conv_taps[0] * padded[:-2] + conv_taps[1] * padded[1:-1] + conv_taps[2] * padded[2:]
        conv_out = (outer_gate.astype(jnp.float32) * mixed_conv).astype(jnp.bfloat16)
        attended, log_total = banded_attention(queries, key_proj, value_proj, sink_logit)
        return (attended, conv_out, log_total)
    attn_out, conv_out, log_total = lax.map(one_sequence, tokens)
    return (attn_out, conv_out, log_total)
```

```python
import functools
import math

import jax
import jax.numpy as jnp
from jax import lax
from jax.experimental import pallas as pl
from jax.experimental.pallas import tpu as pltpu
from jax.sharding import PartitionSpec as P

HEAD = 64
WINDOW = 128
EPSILON = 1e-06


def normalized(tokens, norm_gain):
    values = tokens.astype(jnp.float32)
    scaling = lax.rsqrt(jnp.mean(values * values, axis=-1, keepdims=True) + EPSILON)
    return (values * scaling * norm_gain).astype(jnp.bfloat16)


def after(value, *earlier):
    return lax.optimization_barrier((value,) + earlier)[0]


def gathered_pieces(groups):
    sp, fs = lax.axis_size("sp"), lax.axis_size("fs")
    if fs != 2:
        full = [lax.all_gather(g, ("sp", "fs"), axis=0, tiled=True) for g in groups]
        return [[g] for g in full], jnp.zeros((1,), jnp.int32)
    ring = [(i, (i + 1) % sp) for i in range(sp)]
    swap = [(0, 1), (1, 0)]
    held = [[g] for g in groups]
    turns = [(g, s) for g in range(len(groups)) for s in range(1, sp)]
    swaps = [(g, s) for g in range(len(groups)) for s in range(sp)]
    swapped, moved = [], []
    for k, (g, s) in enumerate(swaps):
        gates = swapped[k - 2 : k - 1] if k >= 2 else []
        if k < len(turns):
            tg, ts = turns[k]
            source = held[tg][ts - 1]
            if gates or moved[:-1]:
                source = after(source, *gates, *(moved[-2:-1]))
            moved.append(lax.ppermute(source, "sp", ring))
            held[tg].append(moved[-1])
        source = held[g][s]
        if gates:
            source = after(source, *gates)
        swapped.append(lax.ppermute(source, "fs", swap))
    z, y = lax.axis_index("sp"), lax.axis_index("fs")
    blocks, pieces = [], [[] for _ in groups]
    for s in range(sp):
        home = lax.rem(z - s + sp, sp) * fs
        blocks += [home + y, home + 1 - y]
    for k, (g, s) in enumerate(swaps):
        pieces[g] += [held[g][s], swapped[k]]
    return pieces, jnp.stack(blocks).astype(jnp.int32)


def fetch(blocks_ref, piece_refs, weight, sems):
    rows = piece_refs[0].shape[0]
    copies = []
    for i, piece in enumerate(piece_refs):
        if len(piece_refs) == 1:
            target = weight
        else:
            target = weight.at[pl.ds(pl.multiple_of(blocks_ref[i] * rows, rows), rows)]
        copies.append(pltpu.make_async_copy(piece, target, sems.at[i]))
    for copy in copies:
        copy.start()
    for copy in copies:
        copy.wait()


def times(normed_ref, weight):
    return jnp.dot(normed_ref[...], weight, preferred_element_type=jnp.float32).astype(jnp.bfloat16)


def plain_kernel(count, blocks_ref, normed_ref, *refs):
    out_ref, weight, sems = refs[count:]
    fetch(blocks_ref, refs[:count], weight, sems)
    out_ref[...] = times(normed_ref, weight[...])


def product_kernel(count, blocks_ref, normed_ref, *refs):
    out_ref, weight, sems = refs[count:]
    fetch(blocks_ref, refs[:count], weight, sems)
    cols = out_ref.shape[1]
    inner = times(normed_ref, weight[:, :cols]).astype(jnp.float32)
    signal = times(normed_ref, weight[:, cols:]).astype(jnp.float32)
    out_ref[...] = (inner * signal).astype(jnp.bfloat16)


def conv_kernel(count, blocks_ref, normed_ref, *refs):
    product_ref, before_ref, after_ref, taps_ref, out_ref, weight, sems = refs[count:]
    fetch(blocks_ref, refs[:count], weight, sems)
    outer = times(normed_ref, weight[...]).astype(jnp.float32)
    product = product_ref[...].astype(jnp.float32)
    length = product.shape[0]
    row = lax.broadcasted_iota(jnp.int32, product.shape, 0)
    previous = jnp.where(row == 0, before_ref[...].astype(jnp.float32), pltpu.roll(product, 1, 0))
    following = jnp.where(
        row == length - 1, after_ref[...].astype(jnp.float32), pltpu.roll(product, length - 1, 0)
    )
    mixed = taps_ref[0:1] * previous + taps_ref[1:2] * product + taps_ref[2:3] * following
    out_ref[...] = (outer * mixed).astype(jnp.bfloat16)


def multiply(kernel, name, blocks, normed, pieces, extra, cols):
    count = len(pieces)
    width = pieces[0].shape[1]
    vmem = pl.BlockSpec(memory_space=pltpu.VMEM)
    return pl.pallas_call(
        functools.partial(kernel, count),
        out_shape=jax.ShapeDtypeStruct((normed.shape[0], cols), jnp.bfloat16),
        in_specs=[pl.BlockSpec(memory_space=pltpu.SMEM), vmem]
        + [pl.BlockSpec(memory_space=pl.ANY)] * count
        + [vmem] * len(extra),
        out_specs=vmem,
        scratch_shapes=[
            pltpu.VMEM((normed.shape[1], width), jnp.bfloat16),
            pltpu.SemaphoreType.DMA((count,)),
        ],
        cost_estimate=pl.CostEstimate(
            flops=2 * normed.shape[0] * normed.shape[1] * width,
            bytes_accessed=2 * normed.shape[1] * width,
            transcendentals=0,
        ),
        name=name,
    )(blocks, normed, *pieces, *extra)


def attention_kernel(
    kv_heads, group, edge_ref, slopes_ref, sink_ref, query_ref, kv_ref, out_ref, log_ref, turned
):
    block = pl.program_id(0)
    last = pl.num_programs(0) - 1
    span = 3 * WINDOW
    kv_cols = kv_heads * HEAD

    @pl.when(block == 0)
    def _():
        turned[...] = jnp.transpose(kv_ref[...].astype(jnp.float32)).astype(jnp.bfloat16)

    key_row = lax.broadcasted_iota(jnp.int32, (span, WINDOW), 0)
    distance = jnp.abs(
        lax.broadcasted_iota(jnp.int32, (span, WINDOW), 1) + WINDOW - key_row
    )
    low = jnp.where(jnp.logical_and(block == 0, edge_ref[0] == 1), WINDOW, 0)
    high = jnp.where(jnp.logical_and(block == last, edge_ref[1] == 1), 2 * WINDOW, span)
    inside = (distance <= WINDOW) & (key_row >= low) & (key_row < high)
    distance = jnp.where(inside, distance.astype(jnp.float32), jnp.inf)
    start = pl.multiple_of(block * WINDOW, WINDOW)
    scale = 1.0 / math.sqrt(HEAD)
    for k in range(kv_heads):
        keys = kv_ref[pl.ds(start, span), k * HEAD : (k + 1) * HEAD]
        values = turned[kv_cols + k * HEAD : kv_cols + (k + 1) * HEAD, pl.ds(start, span)]
        queries = jnp.concatenate(
            [query_ref[:, h * HEAD : (h + 1) * HEAD] for h in range(k * group, (k + 1) * group)],
            axis=0,
        )
        scores = lax.dot_general(
            keys, queries, (((1,), (1,)), ((), ())), preferred_element_type=jnp.float32
        )
        rounded, totals = [], []
        for g in range(group):
            h = k * group + g
            own = scores[:, g * WINDOW : (g + 1) * WINDOW] * scale - slopes_ref[h] * distance
            peak = jnp.maximum(jnp.max(own, axis=0, keepdims=True), sink_ref[h])
            weights = jnp.exp(own - peak)
            total = jnp.sum(weights, axis=0, keepdims=True) + jnp.exp(sink_ref[h] - peak)
            log_ref[h : h + 1, :] = peak + jnp.log(total)
            rounded.append(weights.astype(jnp.bfloat16))
            totals.append(total)
        weighted = jnp.dot(
            values, jnp.concatenate(rounded, axis=1), preferred_element_type=jnp.float32
        )
        weighted = weighted / jnp.concatenate(totals, axis=1)
        for g in range(0, group, 2):
            pair = jnp.concatenate(
                [weighted[:, i * WINDOW : (i + 1) * WINDOW] for i in (g, g + 1)], axis=0
            )
            h = k * group + g
            out_ref[:, h * HEAD : (h + 2) * HEAD] = jnp.transpose(pair).astype(jnp.bfloat16)


def attention(queries_cols, projected, kv_rows, edges, slopes, sink_logit):
    tok_count = projected.shape[0]
    kv_heads = kv_rows.shape[1] // (2 * HEAD)
    heads = queries_cols // HEAD
    smem = pl.BlockSpec(memory_space=pltpu.SMEM)
    return pl.pallas_call(
        functools.partial(attention_kernel, kv_heads, heads // kv_heads),
        grid=(tok_count // WINDOW,),
        out_shape=(
            jax.ShapeDtypeStruct((tok_count, queries_cols), jnp.bfloat16),
            jax.ShapeDtypeStruct((heads, tok_count), jnp.float32),
        ),
        in_specs=[
            smem,
            smem,
            smem,
            pl.BlockSpec((WINDOW, queries_cols), lambda b: (b, 0)),
            pl.BlockSpec(memory_space=pltpu.VMEM),
        ],
        out_specs=(
            pl.BlockSpec((WINDOW, queries_cols), lambda b: (b, 0)),
            pl.BlockSpec((heads, WINDOW), lambda b: (0, b)),
        ),
        scratch_shapes=[pltpu.VMEM(kv_rows.shape[::-1], jnp.bfloat16)],
        cost_estimate=pl.CostEstimate(
            flops=12 * tok_count * 3 * WINDOW * queries_cols, bytes_accessed=4 * 2**20,
            transcendentals=tok_count * 3 * WINDOW * heads,
        ),
        name="banded_attention",
    )(edges, slopes, sink_logit, projected, kv_rows)


def neighbours(value, width):
    size, length = lax.axis_size("sp"), value.shape[0]
    up = [(i, i + 1) for i in range(size - 1)]
    before = lax.ppermute(value[length - width :], "sp", up)
    behind = lax.ppermute(value[:width], "sp", [(j, i) for i, j in up])
    return before, behind


def per_device(
    tokens,
    norm_gain,
    query_weight,
    key_weight,
    value_weight,
    outer_weight,
    inner_weight,
    signal_weight,
    conv_taps,
    sink_logit,
):
    groups = [
        jnp.concatenate([query_weight, key_weight, value_weight], axis=1),
        jnp.concatenate([inner_weight, signal_weight], axis=1),
        outer_weight,
    ]
    pieces, blocks = gathered_pieces(groups)
    normed = normalized(tokens[0], norm_gain)
    query_cols, channels = query_weight.shape[1], outer_weight.shape[1]
    tok_count = normed.shape[0]

    projected = multiply(
        plain_kernel, "project", blocks, normed, pieces[0], (), groups[0].shape[1]
    )
    kv_own = projected[:, query_cols:]
    kv_before, kv_behind = neighbours(kv_own, WINDOW)
    kv_rows = jnp.concatenate([kv_before, kv_own, kv_behind], axis=0)
    sp, z = lax.axis_size("sp"), lax.axis_index("sp")
    edges = jnp.stack([z == 0, z == sp - 1]).astype(jnp.int32)
    head_local = query_cols // HEAD
    head_index = lax.axis_index("tp") * head_local + jnp.arange(1, head_local + 1)
    slopes = jnp.exp2(-8.0 * head_index.astype(jnp.float32) / (head_local * lax.axis_size("tp")))
    attended, log_total = attention(query_cols, projected, kv_rows, edges, slopes, sink_logit)

    product = multiply(product_kernel, "gates", blocks, normed, pieces[1], (), channels)
    row_before, row_behind = neighbours(product, 1)
    conv_out = multiply(
        conv_kernel,
        "convolve",
        blocks,
        normed,
        pieces[2],
        (product, row_before, row_behind, conv_taps),
        channels,
    )
    return (attended[None], conv_out[None], log_total[None])


def solution(mesh):
    in_specs = (
        P("fs", "sp", None),
        P(),
        P(("sp", "fs"), "tp"),
        P(("sp", "fs"), "tp"),
        P(("sp", "fs"), "tp"),
        P(("sp", "fs"), "tp"),
        P(("sp", "fs"), "tp"),
        P(("sp", "fs"), "tp"),
        P(None, "tp"),
        P("tp"),
    )
    out_specs = (P("fs", "sp", "tp"), P("fs", "sp", "tp"), P("fs", "tp", "sp"))
    return jax.shard_map(
        per_device, mesh=mesh, in_specs=in_specs, out_specs=out_specs, check_vma=False
    )
```

```python
import functools
import math

import jax
import jax.numpy as jnp
from jax import lax
from jax.experimental import pallas as pl
from jax.experimental.pallas import tpu as pltpu
from jax.sharding import PartitionSpec as P

HEAD = 64
WINDOW = 128
EPSILON = 1e-06


def normalized(tokens, norm_gain):
    values = tokens.astype(jnp.float32)
    scaling = lax.rsqrt(jnp.mean(values * values, axis=-1, keepdims=True) + EPSILON)
    return (values * scaling * norm_gain).astype(jnp.bfloat16)


def after(value, *earlier):
    return lax.optimization_barrier((value,) + earlier)[0]


def gathered_pieces(groups, normed, project):
    sp, fs = lax.axis_size("sp"), lax.axis_size("fs")
    if fs != 2:
        full = [lax.all_gather(g, ("sp", "fs"), axis=0, tiled=True) for g in groups]
        blocks = jnp.zeros((1,), jnp.int32)
        return [[g] for g in full], blocks, project(blocks, full[:1])
    z, y = lax.axis_index("sp"), lax.axis_index("fs")
    blocks = []
    for s in range(sp):
        home = lax.rem(z - s + sp, sp) * fs
        blocks += [home + y, home + 1 - y]
    blocks = jnp.stack(blocks).astype(jnp.int32)
    ring = [(i, (i + 1) % sp) for i in range(sp)]
    swap = [(0, 1), (1, 0)]
    held = {(g, 0, 0): group for g, group in enumerate(groups)}

    first, second, own, other = (
        [(g, side, s) for s in range(1, sp)] for g, side in ((0, 0), (1, 0), (2, 0), (2, 1))
    )
    turns = first[:1] + own[:1] + first[1:2] + other[:1] + first[2:]
    turns += second[:1] + own[1:2] + second[1:] + other[1:2]
    turns += [t for pair in zip(own[2:], other[2:]) for t in pair]
    swaps = [(0, 1, 0), (2, 1, 0)] + [(0, 1, s) for s in range(1, sp)]
    swaps[3:3] = [(1, 1, 0)]
    swaps += [(1, 1, s) for s in range(1, sp)]
    moved, swapped = [], []
    while turns or swaps:
        gates = moved[-2:-1] + swapped[-2:-1]
        if len(moved) == 2:
            gates = gates + [normed]
        if turns:
            g, side, s = turns[0]
            if turns[0] == second[-1]:
                ready = [held[0, i, j] for j in range(sp) for i in range(fs)]
                projected = project(blocks, ready)
                gates = gates + [projected]
            source = held[g, side, s - 1]
            arrived = lax.ppermute(after(source, *gates) if gates else source, "sp", ring)
            moved.append(arrived)
            held[turns.pop(0)] = arrived
        if swaps and (swaps[0][0], 0, swaps[0][2]) in held:
            g, _, s = swaps[0]
            source = held[g, 0, s]
            arrived = lax.ppermute(after(source, *gates) if gates else source, "fs", swap)
            swapped.append(arrived)
            held[swaps.pop(0)] = arrived
    pieces = [
        [held[g, side, s] for s in range(sp) for side in range(fs)] for g in range(len(groups))
    ]
    return pieces, blocks, projected


def fetch(blocks_ref, piece_refs, weight, sems):
    rows = piece_refs[0].shape[0]
    copies = []
    for i, piece in enumerate(piece_refs):
        if len(piece_refs) == 1:
            target = weight
        else:
            target = weight.at[pl.ds(pl.multiple_of(blocks_ref[i] * rows, rows), rows)]
        copies.append(pltpu.make_async_copy(piece, target, sems.at[i]))
    for copy in copies:
        copy.start()
    for copy in copies:
        copy.wait()


def times(normed_ref, weight):
    return jnp.dot(normed_ref[...], weight, preferred_element_type=jnp.float32).astype(jnp.bfloat16)


def plain_kernel(count, blocks_ref, normed_ref, *refs):
    out_ref, weight, sems = refs[count:]
    fetch(blocks_ref, refs[:count], weight, sems)
    out_ref[...] = times(normed_ref, weight[...])


def product_kernel(count, blocks_ref, normed_ref, *refs):
    out_ref, weight, sems = refs[count:]
    fetch(blocks_ref, refs[:count], weight, sems)
    cols = out_ref.shape[1]
    inner = times(normed_ref, weight[:, :cols]).astype(jnp.float32)
    signal = times(normed_ref, weight[:, cols:]).astype(jnp.float32)
    out_ref[...] = (inner * signal).astype(jnp.bfloat16)


def conv_kernel(count, blocks_ref, normed_ref, *refs):
    product_ref, before_ref, after_ref, taps_ref, out_ref, weight, sems = refs[count:]
    fetch(blocks_ref, refs[:count], weight, sems)
    outer = times(normed_ref, weight[...]).astype(jnp.float32)
    product = product_ref[...].astype(jnp.float32)
    length = product.shape[0]
    row = lax.broadcasted_iota(jnp.int32, product.shape, 0)
    previous = jnp.where(row == 0, before_ref[...].astype(jnp.float32), pltpu.roll(product, 1, 0))
    following = jnp.where(
        row == length - 1, after_ref[...].astype(jnp.float32), pltpu.roll(product, length - 1, 0)
    )
    mixed = taps_ref[0:1] * previous + taps_ref[1:2] * product + taps_ref[2:3] * following
    out_ref[...] = (outer * mixed).astype(jnp.bfloat16)


def multiply(kernel, name, blocks, normed, pieces, extra, cols):
    count = len(pieces)
    width = pieces[0].shape[1]
    vmem = pl.BlockSpec(memory_space=pltpu.VMEM)
    return pl.pallas_call(
        functools.partial(kernel, count),
        out_shape=jax.ShapeDtypeStruct((normed.shape[0], cols), jnp.bfloat16),
        in_specs=[pl.BlockSpec(memory_space=pltpu.SMEM), vmem]
        + [pl.BlockSpec(memory_space=pl.ANY)] * count
        + [vmem] * len(extra),
        out_specs=vmem,
        scratch_shapes=[
            pltpu.VMEM((normed.shape[1], width), jnp.bfloat16),
            pltpu.SemaphoreType.DMA((count,)),
        ],
        cost_estimate=pl.CostEstimate(
            flops=2 * normed.shape[0] * normed.shape[1] * width,
            bytes_accessed=2 * normed.shape[1] * width,
            transcendentals=0,
        ),
        name=name,
    )(blocks, normed, *pieces, *extra)


def attention_kernel(
    kv_heads, group, edge_ref, slopes_ref, sink_ref, query_ref, kv_ref, out_ref, log_ref, turned
):
    block = pl.program_id(0)
    last = pl.num_programs(0) - 1
    span = 3 * WINDOW
    kv_cols = kv_heads * HEAD

    @pl.when(block == 0)
    def _():
        turned[...] = jnp.transpose(kv_ref[...].astype(jnp.float32)).astype(jnp.bfloat16)

    key_row = lax.broadcasted_iota(jnp.int32, (span, WINDOW), 0)
    distance = jnp.abs(
        lax.broadcasted_iota(jnp.int32, (span, WINDOW), 1) + WINDOW - key_row
    )
    low = jnp.where(jnp.logical_and(block == 0, edge_ref[0] == 1), WINDOW, 0)
    high = jnp.where(jnp.logical_and(block == last, edge_ref[1] == 1), 2 * WINDOW, span)
    inside = (distance <= WINDOW) & (key_row >= low) & (key_row < high)
    distance = jnp.where(inside, distance.astype(jnp.float32), jnp.inf)
    start = pl.multiple_of(block * WINDOW, WINDOW)
    scale = 1.0 / math.sqrt(HEAD)
    for k in range(kv_heads):
        keys = kv_ref[pl.ds(start, span), k * HEAD : (k + 1) * HEAD]
        values = turned[kv_cols + k * HEAD : kv_cols + (k + 1) * HEAD, pl.ds(start, span)]
        queries = jnp.concatenate(
            [query_ref[:, h * HEAD : (h + 1) * HEAD] for h in range(k * group, (k + 1) * group)],
            axis=0,
        )
        scores = lax.dot_general(
            keys, queries, (((1,), (1,)), ((), ())), preferred_element_type=jnp.float32
        )
        rounded, totals = [], []
        for g in range(group):
            h = k * group + g
            own = scores[:, g * WINDOW : (g + 1) * WINDOW] * scale - slopes_ref[h] * distance
            peak = jnp.maximum(jnp.max(own, axis=0, keepdims=True), sink_ref[h])
            weights = jnp.exp(own - peak)
            total = jnp.sum(weights, axis=0, keepdims=True) + jnp.exp(sink_ref[h] - peak)
            log_ref[h : h + 1, :] = peak + jnp.log(total)
            rounded.append(weights.astype(jnp.bfloat16))
            totals.append(total)
        weighted = jnp.dot(
            values, jnp.concatenate(rounded, axis=1), preferred_element_type=jnp.float32
        )
        weighted = weighted / jnp.concatenate(totals, axis=1)
        for g in range(0, group, 2):
            pair = jnp.concatenate(
                [weighted[:, i * WINDOW : (i + 1) * WINDOW] for i in (g, g + 1)], axis=0
            )
            h = k * group + g
            out_ref[:, h * HEAD : (h + 2) * HEAD] = jnp.transpose(pair).astype(jnp.bfloat16)


def attention(queries_cols, projected, kv_rows, edges, slopes, sink_logit):
    tok_count = projected.shape[0]
    kv_heads = kv_rows.shape[1] // (2 * HEAD)
    heads = queries_cols // HEAD
    smem = pl.BlockSpec(memory_space=pltpu.SMEM)
    return pl.pallas_call(
        functools.partial(attention_kernel, kv_heads, heads // kv_heads),
        grid=(tok_count // WINDOW,),
        out_shape=(
            jax.ShapeDtypeStruct((tok_count, queries_cols), jnp.bfloat16),
            jax.ShapeDtypeStruct((heads, tok_count), jnp.float32),
        ),
        in_specs=[
            smem,
            smem,
            smem,
            pl.BlockSpec((WINDOW, queries_cols), lambda b: (b, 0)),
            pl.BlockSpec(memory_space=pltpu.VMEM),
        ],
        out_specs=(
            pl.BlockSpec((WINDOW, queries_cols), lambda b: (b, 0)),
            pl.BlockSpec((heads, WINDOW), lambda b: (0, b)),
        ),
        scratch_shapes=[pltpu.VMEM(kv_rows.shape[::-1], jnp.bfloat16)],
        cost_estimate=pl.CostEstimate(
            flops=12 * tok_count * 3 * WINDOW * queries_cols, bytes_accessed=4 * 2**20,
            transcendentals=tok_count * 3 * WINDOW * heads,
        ),
        name="banded_attention",
    )(edges, slopes, sink_logit, projected, kv_rows)


def neighbours(value, width):
    size, length = lax.axis_size("sp"), value.shape[0]
    up = [(i, i + 1) for i in range(size - 1)]
    before = lax.ppermute(value[length - width :], "sp", up)
    behind = lax.ppermute(value[:width], "sp", [(j, i) for i, j in up])
    return before, behind


def per_device(
    tokens,
    norm_gain,
    query_weight,
    key_weight,
    value_weight,
    outer_weight,
    inner_weight,
    signal_weight,
    conv_taps,
    sink_logit,
):
    groups = [
        jnp.concatenate([query_weight, key_weight, value_weight], axis=1),
        jnp.concatenate([inner_weight, signal_weight], axis=1),
        outer_weight,
    ]
    normed = normalized(tokens[0], norm_gain)
    width = groups[0].shape[1]
    pieces, blocks, projected = gathered_pieces(
        groups, normed, lambda at, own: multiply(plain_kernel, "project", at, normed, own, (), width)
    )
    query_cols, channels = query_weight.shape[1], outer_weight.shape[1]
    tok_count = normed.shape[0]

    kv_own = projected[:, query_cols:]
    kv_before, kv_behind = neighbours(kv_own, WINDOW)
    kv_rows = jnp.concatenate([kv_before, kv_own, kv_behind], axis=0)
    sp, z = lax.axis_size("sp"), lax.axis_index("sp")
    edges = jnp.stack([z == 0, z == sp - 1]).astype(jnp.int32)
    head_local = query_cols // HEAD
    head_index = lax.axis_index("tp") * head_local + jnp.arange(1, head_local + 1)
    slopes = jnp.exp2(-8.0 * head_index.astype(jnp.float32) / (head_local * lax.axis_size("tp")))
    attended, log_total = attention(query_cols, projected, kv_rows, edges, slopes, sink_logit)

    normed = after(normed, attended)
    product = multiply(product_kernel, "gates", blocks, normed, pieces[1], (), channels)
    row_before, row_behind = neighbours(product, 1)
    conv_out = multiply(
        conv_kernel,
        "convolve",
        blocks,
        normed,
        pieces[2],
        (product, row_before, row_behind, conv_taps),
        channels,
    )
    return (attended[None], conv_out[None], log_total[None])


def solution(mesh):
    in_specs = (
        P("fs", "sp", None),
        P(),
        P(("sp", "fs"), "tp"),
        P(("sp", "fs"), "tp"),
        P(("sp", "fs"), "tp"),
        P(("sp", "fs"), "tp"),
        P(("sp", "fs"), "tp"),
        P(("sp", "fs"), "tp"),
        P(None, "tp"),
        P("tp"),
    )
    out_specs = (P("fs", "sp", "tp"), P("fs", "sp", "tp"), P("fs", "tp", "sp"))
    return jax.shard_map(
        per_device, mesh=mesh, in_specs=in_specs, out_specs=out_specs, check_vma=False
    )
```
